32 devices in a mesh: sp: 4 (over z), fs: 4 (over y, x), tp: 2 (over core).
Axes of the slice: x: 2, y: 2, z: 4, core: 2. Of those that a mesh axis runs over, the one named last changes fastest.
Arguments:
- tokens: bfloat16 [12288, 2048], P(('fs', 'sp'), 'tp'), parts along dimension 0, may hold values from -6 to 6
- norm_gain: bfloat16 [2048], replicated, may hold values from 0.099609375 to 1.8984375
- w_query: bfloat16 [2048, 1024], P(None, 'tp'), may hold values from -0.125 to 0.125
- w_key: bfloat16 [2048, 1024], P(None, 'tp'), may hold values from -0.125 to 0.125
- w_value: bfloat16 [2048, 1024], P(None, 'tp'), may hold values from -0.125 to 0.125
- log_decay: float32 [8, 3072], P('tp', 'sp'), may hold values from -1 to 0
- w_conv_in: bfloat16 [2048, 1024], P(None, 'tp'), may hold values from -0.125 to 0.125
- w_conv_pre: bfloat16 [2048, 1024], P(None, 'tp'), may hold values from -0.125 to 0.125
- w_conv_post: bfloat16 [2048, 1024], P(None, 'tp'), may hold values from -0.125 to 0.125
- conv_taps: bfloat16 [3, 1024], P(None, 'tp'), may hold values from -3 to 3
- w_out_ret: bfloat16 [1024, 2048], replicated, may hold values from -0.125 to 0.125
- w_out_conv: bfloat16 [1024, 2048], replicated, may hold values from -0.125 to 0.125
Outputs:
- mixed: bfloat16 [12288, 2048], P(('fs', 'sp', 'tp')), parts along dimension 0
The draws below stay inside these ranges and needn't reach their ends.
There are 4 independent parts, one for each index of `fs`. The reference program is written for one: setup_inputs(seed, part) draws one part's arguments, and reference() takes and returns one part's arrays. A program takes and returns all parts, laid end to end along the dimension named above; an argument that names none is the same for every part. Nothing has to cross between parts.
All inputs are finite; a program needn't handle non-finite values.
Results may differ from the reference program's by a relative error of at most 0.012.
Values may be sent and summed in bfloat16 or wider, within the bound.
No kernel may reach another device: no remote copies, remote signals or barrier semaphores. Data moves between devices by JAX's collectives and lax.ppermute only.
A program may use at most 128 MiB of HBM per device.

```python
import math
import jax
import jax.numpy as jnp
from jax import lax

D = 2048
RETENTION_HEADS = 8
DH = 128
CW = 1024
TAPS = 3
SPAN = 128
TOK_DEV = 768
SEQUENCE_LENGTH = 3072
RW = 1024


def draw_log_decay(key, part):
    head_order = jax.random.permutation(jax.random.fold_in(key, 1), RETENTION_HEADS)
    fast_heads = head_order < RETENTION_HEADS // 2
    token_position = jnp.arange(SEQUENCE_LENGTH, dtype=jnp.int32)
    segment = token_position // TOK_DEV
    jitter = jax.random.uniform(jax.random.fold_in(key, 2), (SEQUENCE_LENGTH // TOK_DEV,), jnp.float32)
    factor = 2.0 ** (1.5 * (segment % 2).astype(jnp.float32) + 0.5 * jitter[segment])
    slow_scale = jax.random.uniform(jax.random.fold_in(key, 3), (RETENTION_HEADS,), jnp.float32, 0.03, 0.09)
    span_length = jax.random.uniform(jax.random.fold_in(key, 4), (RETENTION_HEADS,), jnp.float32, 50.0, 80.0)
    ln_ten = math.log(10.0)
    fast_rate = ln_ten / span_length[:, None] * factor[None, :] * 0.5
    slow_rate = ln_ten * slow_scale[:, None] * factor[None, :] / SEQUENCE_LENGTH
    decay_speed = jnp.where(fast_heads[:, None], fast_rate, slow_rate)
    spike_position = jax.random.randint(jax.random.fold_in(key, 5), (2,), 0, SEQUENCE_LENGTH)
    spike_penalty = jax.random.uniform(jax.random.fold_in(key, 6), (RETENTION_HEADS, 2), jnp.float32, 0.2, 0.4)
    spike_events = jnp.where(token_position[None, :] == spike_position[0], jnp.log1p(-spike_penalty[:, 0:1]), 0.0)
    spike_events = spike_events + jnp.where(token_position[None, :] == spike_position[1], jnp.log1p(-spike_penalty[:, 1:2]), 0.0)
    return (spike_events - decay_speed).astype(jnp.float32)


def steps_of(stream_key, shape, shards, low, largest):
    loudness = 1.0
    for position, shards_of in shards:
        draws = jax.random.uniform(jax.random.fold_in(jax.random.fold_in(stream_key, 6), position), (shards_of,), jnp.float32, low / len(shards), largest / len(shards))
        loudness = loudness * jnp.repeat(jnp.exp(draws), shape[position] // shards_of).reshape((-1,) + (1,) * (len(shape) - 1 - position))
    return loudness


def normal_values(rng, shape, deviation, bound, cuts=(), kind=jnp.bfloat16):
    gain = steps_of(rng, shape, cuts, -0.22, 0.18) if cuts else 1.0
    result = jax.random.normal(rng, shape, jnp.float32) * deviation * gain
    return jnp.minimum(jnp.maximum(result, -bound), bound).astype(kind)


def setup_inputs(seed: int = 0, part: int = 0) -> dict:
    splits = jax.random.split(jax.random.key(seed), 13)
    own_keys = jax.random.split(jax.random.fold_in(splits[12], part), 13)
    return {
        "tokens": normal_values(own_keys[0], (SEQUENCE_LENGTH, D), 1.0, 6.0, ((0, 4), (1, 2))),
        "norm_gain": jnp.clip(1.0 + 0.18 * jax.random.normal(splits[1], (D,), jnp.float32), 0.099609375, 1.8984375).astype(jnp.bfloat16),
        "w_query": normal_values(splits[2], (D, RW), D ** -0.5, 0.125, ((1, 2),)),
        "w_key": normal_values(splits[3], (D, RW), D ** -0.5, 0.125, ((1, 2),)),
        "w_value": normal_values(splits[4], (D, RW), D ** -0.5, 0.125, ((1, 2),)),
        "log_decay": draw_log_decay(jax.random.fold_in(splits[12], 71), part),
        "w_conv_in": normal_values(splits[6], (D, CW), D ** -0.5, 0.125, ((1, 2),)),
        "w_conv_pre": normal_values(splits[7], (D, CW), D ** -0.5, 0.125, ((1, 2),)),
        "w_conv_post": normal_values(splits[8], (D, CW), D ** -0.5, 0.125, ((1, 2),)),
        "conv_taps": normal_values(splits[9], (TAPS, CW), 0.577, 3.0, ((1, 2),)),
        "w_out_ret": normal_values(splits[10], (RW, D), (RW + CW) ** -0.5, 0.125),
        "w_out_conv": normal_values(splits[11], (CW, D), (RW + CW) ** -0.5, 0.125),
    }


epsilon = 1e-06

def rotate(vectors, positions):
    halfway = vectors.shape[-1] // 2
    inverse = 10000.0 ** (-jnp.arange(halfway, dtype=jnp.float32) / halfway)
    angles = positions.astype(jnp.float32)[:, None] * inverse[None, :]
    cosines = jnp.cos(angles)[:, None, :]
    sinusoid = jnp.sin(angles)[:, None, :]
    leading = vectors[..., :halfway]
    trailing = vectors[..., halfway:]
    return jnp.concatenate([leading * cosines - trailing * sinusoid, leading * sinusoid + trailing * cosines], axis=-1)

def retain(queries, keys, values, log_decay):
    blocks = SEQUENCE_LENGTH // SPAN
    query_blocks = queries.reshape(blocks, SPAN, RETENTION_HEADS, DH)
    key_blocks = keys.reshape(blocks, SPAN, RETENTION_HEADS, DH)
    value_blocks = values.reshape(blocks, SPAN, RETENTION_HEADS, DH)
    decay_blocks = log_decay.reshape(RETENTION_HEADS, blocks, SPAN).transpose(1, 0, 2)
    lower_mask = jnp.tril(jnp.ones((SPAN, SPAN), bool))

    def advance(carried, inputs):
        query_block, key_block, value_block, decay_block = inputs
        cumulative = jnp.cumsum(decay_block, axis=-1)
        differences = cumulative[:, :, None] - cumulative[:, None, :]
        decay_weights = jnp.where(lower_mask[None], jnp.exp(jnp.minimum(differences, 0.0)), 0.0)
        query_float = query_block.astype(jnp.float32)
        key_float = key_block.astype(jnp.float32)
        value_float = value_block.astype(jnp.float32)
        scores = jnp.einsum('shd,thd->hst', query_float, key_float)
        mix_weights = lax.optimization_barrier((scores * decay_weights).astype(jnp.bfloat16)).astype(jnp.float32)
        inside = jnp.einsum('hst,thd->shd', mix_weights, value_float)
        across = jnp.einsum('shd,hde->she', query_float, carried, precision=lax.Precision.HIGHEST)
        retained = inside + jnp.exp(cumulative).T[:, :, None] * across
        last_decay = cumulative[:, -1]
        tail_decay = jnp.exp(last_decay[:, None] - cumulative)
        fresh_state = jnp.einsum('shd,she->hde', key_float, value_float * tail_decay.T[:, :, None], precision=lax.Precision.HIGHEST)
        return (jnp.exp(last_decay)[:, None, None] * carried + fresh_state, retained)
    initial = jnp.zeros((RETENTION_HEADS, DH, DH), jnp.float32)
    unused_state, retained = lax.scan(advance, initial, (query_blocks, key_blocks, value_blocks, decay_blocks))
    retained = retained.reshape(SEQUENCE_LENGTH, RETENTION_HEADS, DH)
    normalized = retained * lax.rsqrt(lax.optimization_barrier(jnp.mean(retained * retained, axis=-1, keepdims=True)) + epsilon)
    return normalized.astype(jnp.bfloat16).reshape(SEQUENCE_LENGTH, RETENTION_HEADS * DH)

def reference(tokens, norm_gain, w_query, w_key, w_value, log_decay, w_conv_in, w_conv_pre, w_conv_post, conv_taps, w_out_ret, w_out_conv):
    floats = tokens.astype(jnp.float32)
    normed = (floats * lax.rsqrt(lax.optimization_barrier(jnp.mean(floats * floats, axis=-1, keepdims=True)) + epsilon) * norm_gain.astype(jnp.float32)).astype(jnp.bfloat16)
    positions = jnp.arange(SEQUENCE_LENGTH, dtype=jnp.int32)

    def project(weight):
        return jnp.dot(normed, weight, preferred_element_type=jnp.float32)
    queries = rotate(project(w_query).reshape(SEQUENCE_LENGTH, RETENTION_HEADS, DH), positions).astype(jnp.bfloat16)
    keys = (rotate(project(w_key).reshape(SEQUENCE_LENGTH, RETENTION_HEADS, DH), positions) * DH ** (-0.5)).astype(jnp.bfloat16)
    values = project(w_value).astype(jnp.bfloat16).reshape(SEQUENCE_LENGTH, RETENTION_HEADS, DH)
    ret_out = retain(queries, keys, values, log_decay)
    conv_in = lax.optimization_barrier(project(w_conv_in).astype(jnp.bfloat16))
    conv_pre = lax.optimization_barrier(project(w_conv_pre).astype(jnp.bfloat16))
    conv_post = lax.optimization_barrier(project(w_conv_post).astype(jnp.bfloat16))
    gated_in = (conv_pre.astype(jnp.float32) * conv_in.astype(jnp.float32)).astype(jnp.bfloat16)
    padded = jnp.pad(gated_in, ((TAPS - 1, 0), (0, 0)))
    convolved = jnp.zeros((SEQUENCE_LENGTH, CW), jnp.float32)
    for tap_index in range(TAPS):
        convolved = convolved + conv_taps[tap_index].astype(jnp.float32) * padded[tap_index:tap_index + SEQUENCE_LENGTH].astype(jnp.float32)
    conv_out = (conv_post.astype(jnp.float32) * convolved).astype(jnp.bfloat16)
    mixed_rows = jnp.dot(ret_out, w_out_ret, preferred_element_type=jnp.float32) + jnp.dot(conv_out, w_out_conv, preferred_element_type=jnp.float32)
    return mixed_rows.astype(jnp.bfloat16)
```

```python
import functools

import jax
import jax.numpy as jnp
from jax import lax
from jax.experimental import pallas as pl
from jax.experimental.pallas import tpu as pltpu
from jax.sharding import PartitionSpec as P

DH = 128
TAPS = 3
SPAN = 128
PACK = 16

epsilon = 1e-06
F32 = jnp.float32
BF16 = jnp.bfloat16


def shifted(value, axis, steps):
    count = lax.axis_size(axis)
    first, last = (max(0, -steps), min(count, count - steps))
    return lax.ppermute(value, axis, [(source, source + steps) for source in range(first, last)])


def swapped(value):
    return lax.ppermute(value, "tp", [(0, 1), (1, 0)])


def turn(vectors, cosines, sines):
    return vectors * cosines + pltpu.roll(vectors, DH // 2, 1) * sines


def contract(left, right, dims):
    return lax.dot_general(left, right, (dims, ((), ())), preferred_element_type=F32)


def call(kernel, grid, in_specs, out_specs, out_shape, flops, scratch=(), limit=28):
    return pl.pallas_call(
        kernel,
        grid_spec=pltpu.PrefetchScalarGridSpec(
            num_scalar_prefetch=1,
            grid=grid,
            in_specs=in_specs,
            out_specs=out_specs,
            scratch_shapes=list(scratch),
        ),
        out_shape=out_shape,
        cost_estimate=pl.CostEstimate(flops=flops, bytes_accessed=flops // 400, transcendentals=0),
        compiler_params=pltpu.CompilerParams(
            dimension_semantics=("arbitrary",) * len(grid), vmem_limit_bytes=limit * 2**20
        ),
    )


def key_value_kernel(chunk, pair, own, other, gain, w_key, w_value, cosines, sines, cum_col,
                     normed, keys, values, starts, total):
    step = pl.program_id(0)
    rows = normed.shape[0]
    half = own.shape[1]

    @pl.when(step == 0)
    def _():
        for begin in range(0, rows, SPAN):
            rng = pl.ds(begin, SPAN)
            mine = own[rng, :].astype(F32)
            theirs = other[rng, :].astype(F32)
            square = jnp.sum(mine * mine + theirs * theirs, axis=-1, keepdims=True)
            scale = lax.rsqrt(square / (2 * half) + epsilon)
            first = pair[0] == 0
            low = jnp.where(first, mine, theirs)
            high = jnp.where(first, theirs, mine)
            normed[rng, :half] = (low * scale * gain[:, :half].astype(F32)).astype(BF16)
            normed[rng, half:] = (high * scale * gain[:, half:].astype(F32)).astype(BF16)

    projected_keys = jnp.dot(normed[...], w_key[...], preferred_element_type=F32)
    projected_values = jnp.dot(normed[...], w_value[...], preferred_element_type=F32)
    values[...] = projected_values.astype(BF16)
    for head in range(w_key.shape[1] // DH):
        lanes = slice(head * DH, (head + 1) * DH)
        turned = turn(projected_keys[:, lanes], cosines[...], sines[...]) * DH ** (-0.5)
        turned = turned.astype(BF16)
        keys[:, lanes] = turned
        state = jnp.zeros((DH, DH), F32)
        decay = jnp.ones((1, 1), F32)
        for index in range(rows // chunk):
            begin = index * chunk
            cum = cum_col[0, begin : begin + chunk, head : head + 1]
            end = cum_col[0, begin + chunk - 1 : begin + chunk, head : head + 1]
            starts[head, index] = state.astype(BF16)
            piece = projected_values[begin : begin + chunk, lanes].astype(BF16).astype(F32)
            weighted = (piece * jnp.exp(end - cum)).astype(BF16)
            state = jnp.exp(end) * state + contract(
                turned[begin : begin + chunk], weighted, ((0,), (0,))
            )
            decay = decay * jnp.exp(end)
        total[head, :DH, :] = state.astype(BF16)
        total[head, DH:, :] = jnp.broadcast_to(decay, (PACK, DH)).astype(BF16)


def gate_kernel(pair, normed, w_in, w_pre, gated):
    entered = jnp.dot(normed[...], w_in[...], preferred_element_type=F32).astype(BF16)
    gate = jnp.dot(normed[...], w_pre[...], preferred_element_type=F32).astype(BF16)
    gated[...] = (gate.astype(F32) * entered.astype(F32)).astype(BF16)


def local_kernel(chunk, pair, normed, w_query, w_post, keys, values, starts, cosines, sines,
                 cum_col, cum_row, queries, local, post):
    rows = normed.shape[0]
    projected = jnp.dot(normed[...], w_query[...], preferred_element_type=F32)
    t_index = lax.broadcasted_iota(jnp.int32, (chunk, chunk), 0)
    s_index = lax.broadcasted_iota(jnp.int32, (chunk, chunk), 1)
    mask = t_index >= s_index
    for head in range(w_query.shape[1] // DH):
        lanes = slice(head * DH, (head + 1) * DH)
        turned = turn(projected[:, lanes], cosines[...], sines[...]).astype(BF16)
        queries[:, lanes] = turned
        for index in range(rows // chunk):
            begin = index * chunk
            rng = slice(begin, begin + chunk)
            query = turned[rng]
            column = cum_col[0, rng, head : head + 1]
            row = cum_row[0, head : head + 1, rng]
            scores = contract(query, keys[rng, lanes], ((1,), (1,)))
            decays = jnp.where(mask, jnp.exp(jnp.minimum(column - row, 0.0)), 0.0)
            mixing = (scores * decays).astype(BF16)
            inside = jnp.dot(mixing, values[rng, lanes], preferred_element_type=F32)
            if index:
                across = jnp.dot(query, starts[head, index], preferred_element_type=F32)
                inside = inside + jnp.exp(column) * across
            local[rng, lanes] = inside
    post[...] = jnp.dot(normed[...], w_post[...], preferred_element_type=F32).astype(BF16)


def finish_kernel(rounds, which, queries, local, reach, gated, before, rim, post, taps, *rest):
    received = rest[:rounds]
    merged = rest[rounds]
    rows = queries.shape[0]
    width = queries.shape[1]
    for head in range(width // DH):
        lanes = slice(head * DH, (head + 1) * DH)
        incoming = received[0][head, :DH, :].astype(F32)
        reached = received[0][head, DH : DH + 1, :].astype(F32)
        for message in received[1:]:
            incoming = incoming + reached * message[head, :DH, :].astype(F32)
            reached = reached * message[head, DH : DH + 1, :].astype(F32)
        across = jnp.dot(queries[:, lanes], incoming.astype(BF16), preferred_element_type=F32)
        retained = local[:, lanes] + reach[:, head : head + 1] * across
        square = jnp.mean(retained * retained, axis=-1, keepdims=True)
        merged[:, lanes] = (retained * lax.rsqrt(square + epsilon)).astype(BF16)
    current = gated[...].astype(F32)
    previous = jnp.where(which[0] == 0, rim[...].astype(F32), before[...].astype(F32))
    extended = jnp.concatenate([previous[PACK - 8 :], current], axis=0)
    convolved = taps[TAPS - 1 : TAPS, :].astype(F32) * current
    for tap in range(TAPS - 1):
        offset = 8 - (TAPS - 1) + tap
        convolved = convolved + taps[tap : tap + 1, :].astype(F32) * extended[offset : offset + rows]
    merged[:, width:] = (post[...].astype(F32) * convolved).astype(BF16)


def first_kernel(which, merged, w_ret, w_conv, partial):
    width = w_ret.shape[0]
    partial[...] = jnp.dot(
        merged[:, :width], w_ret[...], preferred_element_type=F32
    ) + jnp.dot(merged[:, width:], w_conv[...], preferred_element_type=F32)


def second_kernel(which, merged, w_ret, w_conv, partial, mixed):
    width = w_ret.shape[0]
    mixed[...] = (
        partial[...]
        + jnp.dot(merged[:, :width], w_ret[...], preferred_element_type=F32)
        + jnp.dot(merged[:, width:], w_conv[...], preferred_element_type=F32)
    ).astype(BF16)


def body(
    tokens,
    norm_gain,
    w_query,
    w_key,
    w_value,
    log_decay,
    w_conv_in,
    w_conv_pre,
    w_conv_post,
    conv_taps,
    w_out_ret,
    w_out_conv,
):
    other = swapped(tokens)
    rows, half = tokens.shape
    depth = 2 * half
    width = w_query.shape[1]
    conv_width = w_conv_in.shape[1]
    heads = width // DH
    chunk = 2 * SPAN if rows % (2 * SPAN) == 0 else SPAN
    chunks = rows // chunk
    group = 2 if heads % 2 == 0 else 1
    steps = heads // group
    gw = group * DH
    cgw = conv_width // steps
    pair = lax.axis_index("tp").astype(jnp.int32)
    pair_scalar = pair.reshape(1)

    halfway = DH // 2
    positions = lax.axis_index("sp") * rows + jnp.arange(rows, dtype=jnp.int32)
    inverse = 10000.0 ** (-jnp.arange(halfway, dtype=F32) / halfway)
    angles = positions.astype(F32)[:, None] * jnp.concatenate([inverse, inverse])[None, :]
    sign = jnp.where(jnp.arange(DH) < halfway, -1.0, 1.0).astype(F32)
    cosines = jnp.cos(angles)
    sines = jnp.sin(angles) * sign[None, :]

    cumulative = jnp.cumsum(log_decay.reshape(heads, chunks, chunk), axis=-1)
    ends = cumulative[..., -1]
    prefix = jnp.cumsum(ends, axis=-1) - ends
    reach = jnp.exp(cumulative + prefix[..., None]).reshape(heads, rows).T
    cum_row = cumulative.reshape(steps, group, rows)
    cum_col = cum_row.transpose(0, 2, 1)

    full = lambda *shape: pl.BlockSpec(shape, lambda j, s: (0,) * len(shape))
    columns = lambda height, size: pl.BlockSpec((height, size), lambda j, s: (0, j))
    lead = lambda *shape: pl.BlockSpec(shape, lambda j, s: (j,) + (0,) * (len(shape) - 1))
    arr = jax.ShapeDtypeStruct
    unit = 2 * rows * depth * width

    normed, keys, values, starts, total = call(
        functools.partial(key_value_kernel, chunk),
        (steps,),
        [full(rows, half), full(rows, half), full(1, depth), columns(depth, gw), columns(depth, gw),
         full(rows, DH), full(rows, DH), lead(1, rows, group)],
        [full(rows, depth), columns(rows, gw), columns(rows, gw),
         lead(group, chunks, DH, DH), lead(group, DH + PACK, DH)],
        [arr((rows, depth), BF16), arr((rows, width), BF16), arr((rows, width), BF16),
         arr((heads, chunks, DH, DH), BF16), arr((heads, DH + PACK, DH), BF16)],
        2 * unit,
    )(pair_scalar, tokens, other, norm_gain.reshape(1, depth), w_key, w_value, cosines, sines,
      cum_col)

    gated = call(
        gate_kernel,
        (steps,),
        [full(rows, depth), columns(depth, cgw), columns(depth, cgw)],
        columns(rows, cgw),
        arr((rows, conv_width), BF16),
        2 * unit,
    )(pair_scalar, normed, w_conv_in, w_conv_pre)
    rim = shifted(gated[rows - PACK :], "sp", 1)

    received = []
    window = total
    steps_back = 1
    count = lax.axis_size("sp")
    while steps_back < count or not received:
        message = shifted(window, "sp", steps_back)
        received.append(message)
        steps_back *= 2
        if steps_back < count:
            own_decay = window[:, DH : DH + 1, :].astype(F32)
            is_state = (jnp.arange(DH + PACK) < DH)[None, :, None]
            window = (
                jnp.where(is_state, window.astype(F32), 0.0) + own_decay * message.astype(F32)
            ).astype(BF16)

    queries, local, post = call(
        functools.partial(local_kernel, chunk),
        (steps,),
        [full(rows, depth), columns(depth, gw), columns(depth, cgw), columns(rows, gw),
         columns(rows, gw), lead(group, chunks, DH, DH), full(rows, DH), full(rows, DH),
         lead(1, rows, group), lead(1, group, rows)],
        [columns(rows, gw), columns(rows, gw), columns(rows, cgw)],
        [arr((rows, width), BF16), arr((rows, width), F32), arr((rows, conv_width), BF16)],
        3 * unit,
    )(pair_scalar, normed, w_query, w_conv_post, keys, values, starts, cosines, sines, cum_col,
      cum_row)

    part = rows // 2
    blocks_per = part // PACK

    def finish(which):
        piece = lambda size: pl.BlockSpec((part, size), lambda j, s: (s[0], 0))
        return call(
            functools.partial(finish_kernel, len(received)),
            (1,),
            [piece(width), piece(width), piece(heads), piece(conv_width),
             pl.BlockSpec(
                 (PACK, conv_width), lambda j, s: (jnp.maximum(s[0] * blocks_per - 1, 0), 0)
             ),
             full(PACK, conv_width), piece(conv_width), full(TAPS, conv_width)]
            + [full(heads, DH + PACK, DH)] * len(received),
            full(part, width + conv_width),
            arr((part, width + conv_width), BF16),
            unit // 3,
        )(which.reshape(1), queries, local, reach, gated, gated, rim, post, conv_taps, *received)

    to_send = finish(1 - pair)
    arrived = swapped(to_send)
    kept = finish(pair)

    model = w_out_ret.shape[1]
    tile = model // 4
    weight = lambda height: pl.BlockSpec((height, tile), lambda j, s: (s[0], j))
    partial = call(
        first_kernel,
        (model // tile,),
        [full(part, width + conv_width), weight(width), weight(conv_width)],
        columns(part, tile),
        arr((part, model), F32),
        unit,
    )(pair_scalar, kept, w_out_ret, w_out_conv)
    return call(
        second_kernel,
        (model // tile,),
        [full(part, width + conv_width), weight(width), weight(conv_width), columns(part, tile)],
        columns(part, tile),
        arr((part, model), BF16),
        unit,
    )(1 - pair_scalar, arrived, w_out_ret, w_out_conv, partial)


def solution(mesh):
    in_specs = (
        P(("fs", "sp"), "tp"),
        P(),
        P(None, "tp"),
        P(None, "tp"),
        P(None, "tp"),
        P("tp", "sp"),
        P(None, "tp"),
        P(None, "tp"),
        P(None, "tp"),
        P(None, "tp"),
        P(),
        P(),
    )
    out_specs = P(("fs", "sp", "tp"), None)
    return jax.shard_map(body, mesh=mesh, in_specs=in_specs, out_specs=out_specs, check_vma=False)
```

```python
import functools

import jax
import jax.numpy as jnp
from jax import lax
from jax.experimental import pallas as pl
from jax.experimental.pallas import tpu as pltpu
from jax.sharding import PartitionSpec as P

DH = 128
TAPS = 3
SPAN = 128
PACK = 16

epsilon = 1e-06
F32 = jnp.float32
BF16 = jnp.bfloat16


def shifted(value, axis, steps):
    count = lax.axis_size(axis)
    first, last = (max(0, -steps), min(count, count - steps))
    return lax.ppermute(value, axis, [(source, source + steps) for source in range(first, last)])


def swapped(value):
    return lax.ppermute(value, "tp", [(0, 1), (1, 0)])


def turn(vectors, cosines, sines):
    return vectors * cosines + pltpu.roll(vectors, DH // 2, 1) * sines


def contract(left, right, dims):
    return lax.dot_general(left, right, (dims, ((), ())), preferred_element_type=F32)


def call(kernel, grid, in_specs, out_specs, out_shape, flops, scratch=(), limit=28):
    return pl.pallas_call(
        kernel,
        grid_spec=pltpu.PrefetchScalarGridSpec(
            num_scalar_prefetch=1,
            grid=grid,
            in_specs=in_specs,
            out_specs=out_specs,
            scratch_shapes=list(scratch),
        ),
        out_shape=out_shape,
        cost_estimate=pl.CostEstimate(flops=flops, bytes_accessed=flops // 400, transcendentals=0),
        compiler_params=pltpu.CompilerParams(
            dimension_semantics=("arbitrary",) * len(grid), vmem_limit_bytes=limit * 2**20
        ),
    )


def project(pair, normed, weight):
    half = normed.shape[1] // 2
    mine = pl.multiple_of(pair[0] * half, half)
    theirs = pl.multiple_of((1 - pair[0]) * half, half)
    return jnp.dot(
        normed[:, :half], weight[pl.ds(mine, half), :], preferred_element_type=F32
    ) + jnp.dot(normed[:, half:], weight[pl.ds(theirs, half), :], preferred_element_type=F32)


def decay_kernel(chunk, group, pair, log_decay, cum_row, cum_col, reach):
    heads, rows = log_decay.shape
    first = lax.broadcasted_iota(jnp.int32, (chunk, chunk), 0)
    second = lax.broadcasted_iota(jnp.int32, (chunk, chunk), 1)
    upper = (first <= second).astype(F32)
    lower = (first >= second).astype(F32)
    prefix = jnp.zeros((1, heads), F32)
    for begin in range(0, rows, chunk):
        rng = slice(begin, begin + chunk)
        piece = log_decay[:, rng]
        row = jnp.dot(piece, upper, precision=lax.Precision.HIGHEST, preferred_element_type=F32)
        column = lax.dot_general(
            lower, piece, (((1,), (1,)), ((), ())),
            precision=lax.Precision.HIGHEST, preferred_element_type=F32,
        )
        for step in range(heads // group):
            cum_row[step, :, rng] = row[step * group : (step + 1) * group]
            cum_col[step, rng, :] = column[:, step * group : (step + 1) * group]
        reach[rng, :] = jnp.exp(column + prefix)
        prefix = prefix + column[chunk - 1 : chunk, :]


def key_value_kernel(chunk, pair, own, other, gain, w_key, w_value, cosines, sines, cum_col,
                     normed, keys, values, starts, total):
    step = pl.program_id(0)
    rows = normed.shape[0]
    half = own.shape[1]

    @pl.when(step == 0)
    def _():
        low_gain = gain[0:1, :].astype(F32)
        high_gain = gain[1:2, :].astype(F32)
        my_gain = jnp.where(pair[0] == 0, low_gain, high_gain)
        their_gain = jnp.where(pair[0] == 0, high_gain, low_gain)
        for begin in range(0, rows, SPAN):
            rng = pl.ds(begin, SPAN)
            mine = own[rng, :].astype(F32)
            theirs = other[rng, :].astype(F32)
            square = jnp.sum(mine * mine + theirs * theirs, axis=-1, keepdims=True)
            scale = lax.rsqrt(square / (2 * half) + epsilon)
            normed[rng, :half] = (mine * scale * my_gain).astype(BF16)
            normed[rng, half:] = (theirs * scale * their_gain).astype(BF16)

    projected_keys = project(pair, normed, w_key)
    projected_values = project(pair, normed, w_value)
    values[...] = projected_values.astype(BF16)
    for head in range(w_key.shape[1] // DH):
        lanes = slice(head * DH, (head + 1) * DH)
        turned = turn(projected_keys[:, lanes], cosines[...], sines[...]) * DH ** (-0.5)
        turned = turned.astype(BF16)
        keys[:, lanes] = turned
        state = jnp.zeros((DH, DH), F32)
        decay = jnp.ones((1, 1), F32)
        for index in range(rows // chunk):
            begin = index * chunk
            cum = cum_col[0, begin : begin + chunk, head : head + 1]
            end = cum_col[0, begin + chunk - 1 : begin + chunk, head : head + 1]
            starts[head, index] = state.astype(BF16)
            piece = projected_values[begin : begin + chunk, lanes].astype(BF16).astype(F32)
            weighted = (piece * jnp.exp(end - cum)).astype(BF16)
            state = jnp.exp(end) * state + contract(
                turned[begin : begin + chunk], weighted, ((0,), (0,))
            )
            decay = decay * jnp.exp(end)
        total[:DH, lanes] = state.astype(BF16)
        total[DH:, lanes] = jnp.broadcast_to(decay, (PACK, DH)).astype(BF16)


def gate_kernel(pair, normed, w_in, w_pre, total, gated, message):
    entered = project(pair, normed, w_in).astype(BF16)
    gate = project(pair, normed, w_pre).astype(BF16)
    product = (gate.astype(F32) * entered.astype(F32)).astype(BF16)
    gated[...] = product
    message[: DH + PACK, :] = total[...]
    message[DH + PACK :, :] = product[product.shape[0] - PACK :, :]


def query_kernel(pair, normed, w_query, w_post, cosines, sines, queries, post):
    projected = project(pair, normed, w_query)
    for head in range(w_query.shape[1] // DH):
        lanes = slice(head * DH, (head + 1) * DH)
        queries[:, lanes] = turn(projected[:, lanes], cosines[...], sines[...]).astype(BF16)
    post[...] = project(pair, normed, w_post).astype(BF16)


def local_kernel(chunk, pair, queries, keys, values, starts, cum_col, cum_row, local):
    rows = queries.shape[0]
    t_index = lax.broadcasted_iota(jnp.int32, (chunk, chunk), 0)
    s_index = lax.broadcasted_iota(jnp.int32, (chunk, chunk), 1)
    mask = t_index >= s_index
    for head in range(queries.shape[1] // DH):
        lanes = slice(head * DH, (head + 1) * DH)
        for index in range(rows // chunk):
            begin = index * chunk
            rng = slice(begin, begin + chunk)
            query = queries[rng, lanes]
            column = cum_col[0, rng, head : head + 1]
            row = cum_row[0, head : head + 1, rng]
            scores = contract(query, keys[rng, lanes], ((1,), (1,)))
            decays = jnp.where(mask, jnp.exp(jnp.minimum(column - row, 0.0)), 0.0)
            mixing = (scores * decays).astype(BF16)
            inside = jnp.dot(mixing, values[rng, lanes], preferred_element_type=F32)
            if index:
                across = jnp.dot(query, starts[head, index], preferred_element_type=F32)
                inside = inside + jnp.exp(column) * across
            local[rng, lanes] = inside


def finish_kernel(rounds, which, queries, local, reach, gated, before, post, taps, *rest):
    received = rest[:rounds]
    merged = rest[rounds]
    rows = queries.shape[0]
    width = queries.shape[1]
    for head in range(width // DH):
        lanes = slice(head * DH, (head + 1) * DH)
        incoming = received[0][:DH, lanes].astype(F32)
        reached = received[0][DH : DH + 1, lanes].astype(F32)
        for message in received[1:]:
            incoming = incoming + reached * message[:DH, lanes].astype(F32)
            reached = reached * message[DH : DH + 1, lanes].astype(F32)
        across = jnp.dot(queries[:, lanes], incoming.astype(BF16), preferred_element_type=F32)
        retained = local[:, lanes] + reach[:, head : head + 1] * across
        square = jnp.mean(retained * retained, axis=-1, keepdims=True)
        merged[:, lanes] = (retained * lax.rsqrt(square + epsilon)).astype(BF16)
    current = gated[...].astype(F32)
    previous = jnp.where(which[0] == 0, received[0][DH + PACK :, :].astype(F32), before[...].astype(F32))
    extended = jnp.concatenate([previous[PACK - 8 :], current], axis=0)
    convolved = taps[TAPS - 1 : TAPS, :].astype(F32) * current
    for tap in range(TAPS - 1):
        offset = 8 - (TAPS - 1) + tap
        convolved = convolved + taps[tap : tap + 1, :].astype(F32) * extended[offset : offset + rows]
    merged[:, width:] = (post[...].astype(F32) * convolved).astype(BF16)


def output_kernel(pair, kept, arrived, w_ret, w_conv, mixed):
    width = w_ret.shape[0] // 2
    mine = pl.multiple_of(pair[0] * width, width)
    theirs = pl.multiple_of((1 - pair[0]) * width, width)
    mixed[...] = (
        jnp.dot(kept[:, :width], w_ret[pl.ds(mine, width), :], preferred_element_type=F32)
        + jnp.dot(kept[:, width:], w_conv[pl.ds(mine, width), :], preferred_element_type=F32)
        + jnp.dot(arrived[:, :width], w_ret[pl.ds(theirs, width), :], preferred_element_type=F32)
        + jnp.dot(arrived[:, width:], w_conv[pl.ds(theirs, width), :], preferred_element_type=F32)
    ).astype(BF16)


def body(
    tokens,
    norm_gain,
    w_query,
    w_key,
    w_value,
    log_decay,
    w_conv_in,
    w_conv_pre,
    w_conv_post,
    conv_taps,
    w_out_ret,
    w_out_conv,
):
    other = swapped(tokens)
    rows, half = tokens.shape
    depth = 2 * half
    width = w_query.shape[1]
    conv_width = w_conv_in.shape[1]
    heads = width // DH
    chunk = 2 * SPAN if rows % (2 * SPAN) == 0 else SPAN
    chunks = rows // chunk
    group = 2 if heads % 2 == 0 else 1
    steps = heads // group
    gw = group * DH
    cgw = conv_width // steps
    pair = lax.axis_index("tp").astype(jnp.int32)
    pair_scalar = pair.reshape(1)

    halfway = DH // 2
    positions = lax.axis_index("sp") * rows + jnp.arange(rows, dtype=jnp.int32)
    inverse = 10000.0 ** (-jnp.arange(halfway, dtype=F32) / halfway)
    angles = positions.astype(F32)[:, None] * jnp.concatenate([inverse, inverse])[None, :]
    sign = jnp.where(jnp.arange(DH) < halfway, -1.0, 1.0).astype(F32)
    cosines = jnp.cos(angles)
    sines = jnp.sin(angles) * sign[None, :]

    full = lambda *shape: pl.BlockSpec(shape, lambda j, s: (0,) * len(shape))
    columns = lambda height, size: pl.BlockSpec((height, size), lambda j, s: (0, j))
    lead = lambda *shape: pl.BlockSpec(shape, lambda j, s: (j,) + (0,) * (len(shape) - 1))
    arr = jax.ShapeDtypeStruct
    unit = 2 * rows * depth * width

    cum_row, cum_col, reach = call(
        functools.partial(decay_kernel, chunk, group),
        (1,),
        [full(heads, rows)],
        [full(steps, group, rows), full(steps, rows, group), full(rows, heads)],
        [arr((steps, group, rows), F32), arr((steps, rows, group), F32), arr((rows, heads), F32)],
        unit // 8,
    )(pair_scalar, log_decay)

    normed, keys, values, starts, total = call(
        functools.partial(key_value_kernel, chunk),
        (steps,),
        [full(rows, half), full(rows, half), full(2, half), columns(depth, gw), columns(depth, gw),
         full(rows, DH), full(rows, DH), lead(1, rows, group)],
        [full(rows, depth), columns(rows, gw), columns(rows, gw),
         lead(group, chunks, DH, DH), columns(DH + PACK, gw)],
        [arr((rows, depth), BF16), arr((rows, width), BF16), arr((rows, width), BF16),
         arr((heads, chunks, DH, DH), BF16), arr((DH + PACK, width), BF16)],
        2 * unit,
    )(pair_scalar, tokens, other, norm_gain.reshape(2, half), w_key, w_value, cosines, sines,
      cum_col)

    gated, window = call(
        gate_kernel,
        (steps,),
        [full(rows, depth), columns(depth, cgw), columns(depth, cgw), columns(DH + PACK, gw)],
        [columns(rows, cgw), columns(DH + 2 * PACK, gw)],
        [arr((rows, conv_width), BF16), arr((DH + 2 * PACK, width), BF16)],
        2 * unit,
    )(pair_scalar, normed, w_conv_in, w_conv_pre, total)

    received = []
    steps_back = 1
    count = lax.axis_size("sp")
    while steps_back < count or not received:
        message = shifted(window, "sp", steps_back)
        received.append(message)
        steps_back *= 2
        if steps_back < count:
            own_decay = window[DH : DH + 1, :].astype(F32)
            is_state = (jnp.arange(DH + PACK) < DH)[:, None]
            window = (
                jnp.where(is_state, window[: DH + PACK].astype(F32), 0.0)
                + own_decay * message[: DH + PACK].astype(F32)
            ).astype(BF16)

    queries, post = call(
        query_kernel,
        (steps,),
        [full(rows, depth), columns(depth, gw), columns(depth, cgw), full(rows, DH),
         full(rows, DH)],
        [columns(rows, gw), columns(rows, cgw)],
        [arr((rows, width), BF16), arr((rows, conv_width), BF16)],
        2 * unit,
    )(pair_scalar, normed, w_query, w_conv_post, cosines, sines)
    local = call(
        functools.partial(local_kernel, chunk),
        (steps,),
        [columns(rows, gw), columns(rows, gw), columns(rows, gw), lead(group, chunks, DH, DH),
         lead(1, rows, group), lead(1, group, rows)],
        columns(rows, gw),
        arr((rows, width), F32),
        2 * unit,
    )(pair_scalar, queries, keys, values, starts, cum_col, cum_row)

    part = rows // 2
    blocks_per = part // PACK

    def finish(which):
        piece = lambda size: pl.BlockSpec((part, size), lambda j, s: (s[0], 0))
        return call(
            functools.partial(finish_kernel, len(received)),
            (1,),
            [piece(width), piece(width), piece(heads), piece(conv_width),
             pl.BlockSpec(
                 (PACK, conv_width), lambda j, s: (jnp.maximum(s[0] * blocks_per - 1, 0), 0)
             ),
             piece(conv_width), full(TAPS, conv_width)]
            + [full(*message.shape) for message in received],
            full(part, width + conv_width),
            arr((part, width + conv_width), BF16),
            unit // 3,
        )(which.reshape(1), queries, local, reach, gated, gated, post, conv_taps, *received)

    to_send = finish(1 - pair)
    arrived = swapped(to_send)
    kept = finish(pair)

    model = w_out_ret.shape[1]
    tile = model // 4
    merged_width = width + conv_width
    return call(
        output_kernel,
        (model // tile,),
        [full(part, merged_width), full(part, merged_width),
         columns(w_out_ret.shape[0], tile), columns(w_out_conv.shape[0], tile)],
        columns(part, tile),
        arr((part, model), BF16),
        2 * unit,
    )(pair_scalar, kept, arrived, w_out_ret, w_out_conv)


def solution(mesh):
    in_specs = (
        P(("fs", "sp"), "tp"),
        P(),
        P(None, "tp"),
        P(None, "tp"),
        P(None, "tp"),
        P("tp", "sp"),
        P(None, "tp"),
        P(None, "tp"),
        P(None, "tp"),
        P(None, "tp"),
        P(),
        P(),
    )
    out_specs = P(("fs", "sp", "tp"), None)
    return jax.shard_map(body, mesh=mesh, in_specs=in_specs, out_specs=out_specs, check_vma=False)
```

```python
import functools

import jax
import jax.numpy as jnp
from jax import lax
from jax.experimental import pallas as pl
from jax.experimental.pallas import tpu as pltpu
from jax.sharding import PartitionSpec as P

DH = 128
TAPS = 3
SPAN = 128
PACK = 16

epsilon = 1e-06
F32 = jnp.float32
BF16 = jnp.bfloat16


def shifted(value, axis, steps):
    count = lax.axis_size(axis)
    first, last = (max(0, -steps), min(count, count - steps))
    return lax.ppermute(value, axis, [(source, source + steps) for source in range(first, last)])


def swapped(value):
    return lax.ppermute(value, "tp", [(0, 1), (1, 0)])


def turn(vectors, cosines, sines):
    return vectors * cosines + pltpu.roll(vectors, DH // 2, 1) * sines


def held(value):
    return pltpu.with_memory_space_constraint(value, pltpu.HBM)


def contract(left, right, dims):
    return lax.dot_general(left, right, (dims, ((), ())), preferred_element_type=F32)


def call(kernel, grid, in_specs, out_specs, out_shape, flops, scratch=(), limit=28):
    return pl.pallas_call(
        kernel,
        grid_spec=pltpu.PrefetchScalarGridSpec(
            num_scalar_prefetch=1,
            grid=grid,
            in_specs=in_specs,
            out_specs=out_specs,
            scratch_shapes=list(scratch),
        ),
        out_shape=out_shape,
        cost_estimate=pl.CostEstimate(flops=flops, bytes_accessed=flops // 400, transcendentals=0),
        compiler_params=pltpu.CompilerParams(
            dimension_semantics=("arbitrary",) * len(grid), vmem_limit_bytes=limit * 2**20
        ),
    )


def project(pair, normed, weight):
    half = normed.shape[1] // 2
    mine = pl.multiple_of(pair[0] * half, half)
    theirs = pl.multiple_of((1 - pair[0]) * half, half)
    return jnp.dot(
        normed[:, :half], weight[pl.ds(mine, half), :], preferred_element_type=F32
    ) + jnp.dot(normed[:, half:], weight[pl.ds(theirs, half), :], preferred_element_type=F32)


def decay_kernel(chunk, group, pair, log_decay, cum_row, cum_col, reach):
    heads, rows = log_decay.shape
    first = lax.broadcasted_iota(jnp.int32, (chunk, chunk), 0)
    second = lax.broadcasted_iota(jnp.int32, (chunk, chunk), 1)
    upper = (first <= second).astype(F32)
    lower = (first >= second).astype(F32)
    prefix = jnp.zeros((1, heads), F32)
    for begin in range(0, rows, chunk):
        rng = slice(begin, begin + chunk)
        piece = log_decay[:, rng]
        row = jnp.dot(piece, upper, precision=lax.Precision.HIGHEST, preferred_element_type=F32)
        column = lax.dot_general(
            lower, piece, (((1,), (1,)), ((), ())),
            precision=lax.Precision.HIGHEST, preferred_element_type=F32,
        )
        for step in range(heads // group):
            cum_row[step, :, rng] = row[step * group : (step + 1) * group]
            cum_col[step, rng, :] = column[:, step * group : (step + 1) * group]
        reach[rng, :] = jnp.exp(column + prefix)
        prefix = prefix + column[chunk - 1 : chunk, :]


def key_value_kernel(chunk, pair, own_far, other, gain, key_far, value_far, cosines, sines,
                     cum_col, normed, keys, values, starts, total, own, key_near, value_near,
                     arrivals):
    step = pl.program_id(0)
    rows = normed.shape[0]
    half = own.shape[1]
    steps = key_near.shape[0]
    size = key_near.shape[2]

    def fetches(index):
        lanes = pl.ds(index * size, size)
        return (
            pltpu.make_async_copy(key_far.at[:, lanes], key_near.at[index], arrivals.at[0, index]),
            pltpu.make_async_copy(
                value_far.at[:, lanes], value_near.at[index], arrivals.at[1, index]
            ),
        )

    @pl.when(step == 0)
    def _():
        fetch_own = pltpu.make_async_copy(own_far, own, arrivals.at[2, 0])
        fetch_own.start()
        for index in range(steps):
            for fetch in fetches(index):
                fetch.start()
        fetch_own.wait()
        low_gain = gain[0:1, :].astype(F32)
        high_gain = gain[1:2, :].astype(F32)
        my_gain = jnp.where(pair[0] == 0, low_gain, high_gain)
        their_gain = jnp.where(pair[0] == 0, high_gain, low_gain)
        for begin in range(0, rows, SPAN):
            rng = pl.ds(begin, SPAN)
            mine = own[rng, :].astype(F32)
            theirs = other[rng, :].astype(F32)
            square = jnp.sum(mine * mine + theirs * theirs, axis=-1, keepdims=True)
            scale = lax.rsqrt(square / (2 * half) + epsilon)
            normed[rng, :half] = (mine * scale * my_gain).astype(BF16)
            normed[rng, half:] = (theirs * scale * their_gain).astype(BF16)

    for index in range(steps):

        @pl.when(step == index)
        def _(index=index):
            for fetch in fetches(index):
                fetch.wait()

    projected_keys = project(pair, normed, key_near.at[step])
    projected_values = project(pair, normed, value_near.at[step])
    values[...] = projected_values.astype(BF16)
    for head in range(size // DH):
        lanes = slice(head * DH, (head + 1) * DH)
        turned = turn(projected_keys[:, lanes], cosines[...], sines[...]) * DH ** (-0.5)
        turned = turned.astype(BF16)
        keys[:, lanes] = turned
        state = jnp.zeros((DH, DH), F32)
        decay = jnp.ones((1, 1), F32)
        for index in range(rows // chunk):
            begin = index * chunk
            cum = cum_col[0, begin : begin + chunk, head : head + 1]
            end = cum_col[0, begin + chunk - 1 : begin + chunk, head : head + 1]
            starts[head, index] = state.astype(BF16)
            piece = projected_values[begin : begin + chunk, lanes].astype(BF16).astype(F32)
            weighted = (piece * jnp.exp(end - cum)).astype(BF16)
            state = jnp.exp(end) * state + contract(
                turned[begin : begin + chunk], weighted, ((0,), (0,))
            )
            decay = decay * jnp.exp(end)
        total[:DH, lanes] = state.astype(BF16)
        total[DH:, lanes] = jnp.broadcast_to(decay, (PACK, DH)).astype(BF16)


def gate_kernel(pair, normed, w_in, w_pre, total, gated, message):
    entered = project(pair, normed, w_in).astype(BF16)
    gate = project(pair, normed, w_pre).astype(BF16)
    product = (gate.astype(F32) * entered.astype(F32)).astype(BF16)
    gated[...] = product
    message[: DH + PACK, :] = total[...]
    message[DH + PACK :, :] = product[product.shape[0] - PACK :, :]


def query_kernel(pair, normed, w_query, w_post, cosines, sines, queries, post):
    projected = project(pair, normed, w_query)
    for head in range(w_query.shape[1] // DH):
        lanes = slice(head * DH, (head + 1) * DH)
        queries[:, lanes] = turn(projected[:, lanes], cosines[...], sines[...]).astype(BF16)
    post[...] = project(pair, normed, w_post).astype(BF16)


def local_kernel(chunk, pair, queries, keys, values, starts, cum_col, cum_row, local):
    rows = queries.shape[0]
    t_index = lax.broadcasted_iota(jnp.int32, (chunk, chunk), 0)
    s_index = lax.broadcasted_iota(jnp.int32, (chunk, chunk), 1)
    mask = t_index >= s_index
    for head in range(queries.shape[1] // DH):
        lanes = slice(head * DH, (head + 1) * DH)
        for index in range(rows // chunk):
            begin = index * chunk
            rng = slice(begin, begin + chunk)
            query = queries[rng, lanes]
            column = cum_col[0, rng, head : head + 1]
            row = cum_row[0, head : head + 1, rng]
            scores = contract(query, keys[rng, lanes], ((1,), (1,)))
            decays = jnp.where(mask, jnp.exp(jnp.minimum(column - row, 0.0)), 0.0)
            mixing = (scores * decays).astype(BF16)
            inside = jnp.dot(mixing, values[rng, lanes], preferred_element_type=F32)
            if index:
                across = jnp.dot(query, starts[head, index], preferred_element_type=F32)
                inside = inside + jnp.exp(column) * across
            local[rng, lanes] = inside


def finish_kernel(rounds, which, queries, local, reach, gated, before, post, taps, *rest):
    received = rest[:rounds]
    merged = rest[rounds]
    rows = queries.shape[0]
    width = queries.shape[1]
    for head in range(width // DH):
        lanes = slice(head * DH, (head + 1) * DH)
        incoming = received[0][:DH, lanes].astype(F32)
        reached = received[0][DH : DH + 1, lanes].astype(F32)
        for message in received[1:]:
            incoming = incoming + reached * message[:DH, lanes].astype(F32)
            reached = reached * message[DH : DH + 1, lanes].astype(F32)
        across = jnp.dot(queries[:, lanes], incoming.astype(BF16), preferred_element_type=F32)
        retained = local[:, lanes] + reach[:, head : head + 1] * across
        square = jnp.mean(retained * retained, axis=-1, keepdims=True)
        merged[:, lanes] = (retained * lax.rsqrt(square + epsilon)).astype(BF16)
    current = gated[...].astype(F32)
    previous = jnp.where(which[0] == 0, received[0][DH + PACK :, :].astype(F32), before[...].astype(F32))
    extended = jnp.concatenate([previous[PACK - 8 :], current], axis=0)
    convolved = taps[TAPS - 1 : TAPS, :].astype(F32) * current
    for tap in range(TAPS - 1):
        offset = 8 - (TAPS - 1) + tap
        convolved = convolved + taps[tap : tap + 1, :].astype(F32) * extended[offset : offset + rows]
    merged[:, width:] = (post[...].astype(F32) * convolved).astype(BF16)


def output_kernel(pair, kept, arrived, w_ret, w_conv, mixed):
    width = w_ret.shape[0] // 2
    tile = mixed.shape[1]
    lanes = pl.ds(pl.multiple_of(pl.program_id(0) * tile, tile), tile)
    mine = pl.ds(pl.multiple_of(pair[0] * width, width), width)
    theirs = pl.ds(pl.multiple_of((1 - pair[0]) * width, width), width)
    mixed[...] = (
        jnp.dot(kept[:, :width], w_ret[mine, lanes], preferred_element_type=F32)
        + jnp.dot(kept[:, width:], w_conv[mine, lanes], preferred_element_type=F32)
        + jnp.dot(arrived[:, :width], w_ret[theirs, lanes], preferred_element_type=F32)
        + jnp.dot(arrived[:, width:], w_conv[theirs, lanes], preferred_element_type=F32)
    ).astype(BF16)


def body(
    tokens,
    norm_gain,
    w_query,
    w_key,
    w_value,
    log_decay,
    w_conv_in,
    w_conv_pre,
    w_conv_post,
    conv_taps,
    w_out_ret,
    w_out_conv,
):
    other = swapped(tokens)
    rows, half = tokens.shape
    depth = 2 * half
    width = w_query.shape[1]
    conv_width = w_conv_in.shape[1]
    heads = width // DH
    chunk = 2 * SPAN if rows % (2 * SPAN) == 0 else SPAN
    chunks = rows // chunk
    group = 2 if heads % 2 == 0 else 1
    steps = heads // group
    gw = group * DH
    cgw = conv_width // steps
    pair = lax.axis_index("tp").astype(jnp.int32)
    pair_scalar = pair.reshape(1)

    halfway = DH // 2
    positions = lax.axis_index("sp") * rows + jnp.arange(rows, dtype=jnp.int32)
    inverse = 10000.0 ** (-jnp.arange(halfway, dtype=F32) / halfway)
    angles = positions.astype(F32)[:, None] * jnp.concatenate([inverse, inverse])[None, :]
    sign = jnp.where(jnp.arange(DH) < halfway, -1.0, 1.0).astype(F32)
    cosines = jnp.cos(angles)
    sines = jnp.sin(angles) * sign[None, :]

    full = lambda *shape: pl.BlockSpec(shape, lambda j, s: (0,) * len(shape))
    columns = lambda height, size: pl.BlockSpec((height, size), lambda j, s: (0, j))
    lead = lambda *shape: pl.BlockSpec(shape, lambda j, s: (j,) + (0,) * (len(shape) - 1))
    far = pl.BlockSpec(memory_space=pltpu.HBM)
    near = pl.BlockSpec(memory_space=pltpu.VMEM)
    arr = jax.ShapeDtypeStruct
    unit = 2 * rows * depth * width

    cum_row, cum_col, reach = call(
        functools.partial(decay_kernel, chunk, group),
        (1,),
        [full(heads, rows)],
        [full(steps, group, rows), full(steps, rows, group), full(rows, heads)],
        [arr((steps, group, rows), F32), arr((steps, rows, group), F32), arr((rows, heads), F32)],
        unit // 8,
    )(pair_scalar, log_decay)

    normed, keys, values, starts, total = call(
        functools.partial(key_value_kernel, chunk),
        (steps,),
        [far, full(rows, half), full(2, half), far, far,
         full(rows, DH), full(rows, DH), lead(1, rows, group)],
        [full(rows, depth), columns(rows, gw), columns(rows, gw),
         lead(group, chunks, DH, DH), columns(DH + PACK, gw)],
        [arr((rows, depth), BF16), arr((rows, width), BF16), arr((rows, width), BF16),
         arr((heads, chunks, DH, DH), BF16), arr((DH + PACK, width), BF16)],
        2 * unit,
        [pltpu.VMEM((rows, half), BF16), pltpu.VMEM((steps, depth, gw), BF16),
         pltpu.VMEM((steps, depth, gw), BF16), pltpu.SemaphoreType.DMA((3, steps))],
    )(pair_scalar, held(tokens), other, norm_gain.reshape(2, half), held(w_key), held(w_value),
      cosines, sines, cum_col)

    gated, window = call(
        gate_kernel,
        (steps,),
        [full(rows, depth), columns(depth, cgw), columns(depth, cgw), columns(DH + PACK, gw)],
        [columns(rows, cgw), columns(DH + 2 * PACK, gw)],
        [arr((rows, conv_width), BF16), arr((DH + 2 * PACK, width), BF16)],
        2 * unit,
    )(pair_scalar, normed, w_conv_in, w_conv_pre, total)

    received = []
    steps_back = 1
    count = lax.axis_size("sp")
    while steps_back < count or not received:
        message = shifted(window, "sp", steps_back)
        received.append(message)
        steps_back *= 2
        if steps_back < count:
            own_decay = window[DH : DH + 1, :].astype(F32)
            is_state = (jnp.arange(DH + PACK) < DH)[:, None]
            window = (
                jnp.where(is_state, window[: DH + PACK].astype(F32), 0.0)
                + own_decay * message[: DH + PACK].astype(F32)
            ).astype(BF16)

    queries, post = call(
        query_kernel,
        (steps,),
        [full(rows, depth), columns(depth, gw), columns(depth, cgw), full(rows, DH),
         full(rows, DH)],
        [columns(rows, gw), columns(rows, cgw)],
        [arr((rows, width), BF16), arr((rows, conv_width), BF16)],
        2 * unit,
    )(pair_scalar, normed, w_query, w_conv_post, cosines, sines)
    local = call(
        functools.partial(local_kernel, chunk),
        (steps,),
        [columns(rows, gw), columns(rows, gw), columns(rows, gw), lead(group, chunks, DH, DH),
         lead(1, rows, group), lead(1, group, rows)],
        columns(rows, gw),
        arr((rows, width), F32),
        2 * unit,
    )(pair_scalar, queries, keys, values, starts, cum_col, cum_row)

    part = rows // 2
    blocks_per = part // PACK

    def finish(which):
        piece = lambda size: pl.BlockSpec((part, size), lambda j, s: (s[0], 0))
        return call(
            functools.partial(finish_kernel, len(received)),
            (1,),
            [piece(width), piece(width), piece(heads), piece(conv_width),
             pl.BlockSpec(
                 (PACK, conv_width), lambda j, s: (jnp.maximum(s[0] * blocks_per - 1, 0), 0)
             ),
             piece(conv_width), full(TAPS, conv_width)]
            + [full(*message.shape) for message in received],
            full(part, width + conv_width),
            arr((part, width + conv_width), BF16),
            unit // 3,
        )(which.reshape(1), queries, local, reach, gated, gated, post, conv_taps, *received)

    to_send = finish(1 - pair)
    arrived = swapped(to_send)
    kept = finish(pair)

    model = w_out_ret.shape[1]
    tile = model // 4
    merged_width = width + conv_width
    return call(
        output_kernel,
        (model // tile,),
        [full(part, merged_width), full(part, merged_width),
         near, near],
        columns(part, tile),
        arr((part, model), BF16),
        2 * unit,
    )(pair_scalar, kept, arrived, w_out_ret, w_out_conv)


def solution(mesh):
    in_specs = (
        P(("fs", "sp"), "tp"),
        P(),
        P(None, "tp"),
        P(None, "tp"),
        P(None, "tp"),
        P("tp", "sp"),
        P(None, "tp"),
        P(None, "tp"),
        P(None, "tp"),
        P(None, "tp"),
        P(),
        P(),
    )
    out_specs = P(("fs", "sp", "tp"), None)
    return jax.shard_map(body, mesh=mesh, in_specs=in_specs, out_specs=out_specs, check_vma=False)
```
